256 devices in a mesh: sp: 16 (over y, x), tp: 16 (over z, core).
Axes of the slice: x: 4, y: 4, z: 8, core: 2. Of those that a mesh axis runs over, the one named last changes fastest.
Arguments:
- residual: bfloat16 [8192, 2048], P(('sp', 'tp')), may hold values from -6 to 6
- queries: bfloat16 [8192, 4096], P('sp', 'tp'), may hold values from -6 to 6
- keys: bfloat16 [8192, 4096], P('sp', 'tp'), may hold values from -6 to 6
- values: bfloat16 [8192, 4096], P('sp', 'tp'), may hold values from -6 to 6
- in_gate: float32 [16, 8192], P('tp', 'sp'), may hold values from -5 to 130
- forget_gate: float32 [16, 8192], P('tp', 'sp'), may hold values from 0 to 16
- doc_ids: int32 [8192], P('sp'), may hold values from 0 to 7, never falling along the last dimension, each value on 1 to 4096 neighbouring positions
- head_gain: float32 [4096], P('tp'), may hold values from 0.1 to 1.9
- out_weight: bfloat16 [4096, 2048], P('tp'), may hold values from -0.09375 to 0.09375
- norm_gain: float32 [2048], replicated, may hold values from 0.1 to 1.9
- route_ids: int32 [8192, 2], P(('sp', 'tp')), may hold values from 0 to 15, all different within a row; in each aligned block of 32 rows (0 to 31, 32 to 63, ...) at most 5 rows name the same one
- route_weights: float32 [8192, 2], P(('sp', 'tp')), may hold values from 0.2 to 1
- gate_proj: bfloat16 [16, 2048, 4096], P('sp', None, 'tp'), may hold values from -0.125 to 0.125
- up_proj: bfloat16 [16, 2048, 4096], P('sp', None, 'tp'), may hold values from -0.125 to 0.125
- down_proj: bfloat16 [16, 4096, 2048], P('sp', 'tp'), may hold values from -0.09375 to 0.09375
Outputs:
- mixed: bfloat16 [8192, 2048], P(('sp', 'tp'))
The draws below stay inside these ranges and needn't reach their ends.
Inputs may be any that keep to these rules, and one draw needn't show every extreme that they name: `route_ids`: each row names 2 different experts. In each aligned block of 32 rows (the rows of one device) no expert is named by more than 5 rows, and in some blocks one expert by exactly 5. `doc_ids`: numbers never fall along the sequence; no document covers more than half of the 8192 positions, and one covers exactly half.
All inputs are finite; a program needn't handle non-finite values.
Results may differ from the reference program's by a relative error of at most 0.018.
Values may be sent and summed in bfloat16 or wider, within the bound.
A program may use at most 64 MiB of HBM per device.

```python
import math
import jax
import jax.numpy as jnp
import numpy as np
from jax import lax

D = 2048
STORE_ATTENDERS = 16
HEAD = 256
EXP_FF = 4096
TOPK = 2
TOK_DEV = 512
MIXER = 4096
TOKENS = 8192
ROWS_DEV = 32
EXPERTS = 16
CAP = 5
DOCS = 8
N_SP = 16
N_TP = 16


def draw_in_gate(key, part):
    base = jax.random.truncated_normal(key, -5.0, 5.0, (STORE_ATTENDERS, TOKENS), jnp.float32)
    return base


def draw_forget_gate(key, part):
    fast_count = STORE_ATTENDERS // 2
    ordering = jax.random.permutation(jax.random.fold_in(key, 21), STORE_ATTENDERS)
    fast = ordering < fast_count
    base_rate = jnp.where(fast, 1.0 / 40.0, 0.3 / TOKENS)
    factor = jnp.exp(jax.random.uniform(jax.random.fold_in(key, 22), (TOKENS // TOK_DEV,), jnp.float32, -0.7, 0.7))
    factor = jnp.repeat(factor, TOK_DEV)
    jitter = jnp.exp(0.5 * jax.random.truncated_normal(jax.random.fold_in(key, 23), -3.0, 3.0, (STORE_ATTENDERS, TOKENS), jnp.float32))
    rate = base_rate[:, None] * factor[None, :] * jitter
    recurrence_outcome = -jnp.log(jnp.expm1(rate))
    capacity_offsets = jax.random.randint(jax.random.fold_in(key, 24), (3,), 0, TOKENS)
    surviving_filter = jax.random.uniform(jax.random.fold_in(key, 25), (3,), jnp.float32, 0.5, 0.8)
    specialist_spike = jnp.log(surviving_filter / (1.0 - surviving_filter))
    recurrence_outcome = recurrence_outcome.at[:, capacity_offsets].set(jnp.broadcast_to(specialist_spike[None, :], (STORE_ATTENDERS, 3)))
    return recurrence_outcome


def steps_of(rng, shape, cuts, smallest, top_value):
    def one(position, shards_of):
        steps = jax.random.uniform(jax.random.fold_in(jax.random.fold_in(rng, 6), position), (shards_of,), jnp.float32, smallest / len(cuts), top_value / len(cuts))
        return jnp.repeat(jnp.exp(steps), shape[position] // shards_of).reshape((-1,) + (1,) * (len(shape) - position - 1))

    level = one(*cuts[0])
    for cut in cuts[1:]:
        level = level * one(*cut)
    return level


def length_profile(amount, total, bound, skew):
    loads = [(1 << 20) // math.isqrt(rank ** skew) + 1 for rank in range(2, amount + 1)]
    spare, given = total - bound - (amount - 1), [1] * (amount - 1)
    while spare > 0:
        candidates = [i for i in range(amount - 1) if given[i] < bound]
        mass, remaining = sum([loads[i] for i in candidates]), spare
        for i in candidates:
            extra = min(bound - given[i], max(1, remaining * loads[i] // mass), spare)
            given[i] = given[i] + extra
            spare = spare - extra
    return np.array([bound] + given)


def uneven_parts(stream_key, amount, total, bound, skew):
    if amount == 2:
        one = jax.random.randint(stream_key, (), max(1, total - bound), min(bound, total - 1) + 1)
        return jnp.stack([one, total - one])
    sizes = jnp.asarray(length_profile(amount, total, bound, skew), jnp.int32)
    couples = (amount - 1) // 2
    source_of, sink = sizes[1:1 + 2 * couples:2], sizes[2:2 + 2 * couples:2]
    slack = jnp.minimum(source_of - 1, bound - sink)
    passed = jax.random.randint(jax.random.fold_in(stream_key, 1), (couples,), 0, 1 << 20) % (slack + 1)
    sizes = sizes.at[1:1 + 2 * couples:2].set(source_of - passed).at[2:2 + 2 * couples:2].set(sink + passed)
    return sizes[jax.random.permutation(jax.random.fold_in(stream_key, 2), amount)]


def shared_out(key, own, number, rows, count, top, bound, skew):
    sequence = jax.random.permutation(key, count)
    crowded, common = load_shares(count, rows * top, bound, skew, True), load_shares(count, rows * top, bound, skew, False)
    places = jnp.arange(count)

    def named(lengths, turn):
        used = int((lengths > 0).sum())
        fixed = max(1, used // 4)
        shifted = fixed + (places - fixed + turn * (used - fixed)) % max(1, count - fixed)
        return jnp.zeros((count,), jnp.int32).at[sequence[jnp.where(places < fixed, places, shifted)]].set(jnp.asarray(lengths, jnp.int32))

    lengths = jnp.where(number % 4 == 0, named(crowded, number // 4), named(common, number - number // 4 - 1))
    mixed = jax.random.permutation(jax.random.fold_in(own, 3), count)
    source_of, taker = mixed[0:count // 2 * 2:2], mixed[1:count // 2 * 2:2]
    slack = jnp.minimum(lengths[source_of] - 1, bound - lengths[taker]) // 2
    slack = jnp.where((source_of == sequence[0]) | (taker == sequence[0]) | (lengths[taker] == 0), 0, jnp.maximum(slack, 0))
    shifted = jax.random.randint(jax.random.fold_in(own, 4), (count // 2,), 0, 1 << 20) % (slack + 1)
    lengths = lengths.at[source_of].add(-shifted).at[taker].add(shifted)
    items = jnp.searchsorted(jnp.cumsum(lengths), jnp.arange(rows * top), side="right").astype(jnp.int32)
    table = items.reshape(top, rows).T
    table = table[jax.random.permutation(jax.random.fold_in(own, 1), rows)]
    turn = jax.random.randint(jax.random.fold_in(own, 2), (rows, 1), 0, top)
    return jnp.take_along_axis(table, (jnp.arange(top)[None, :] + turn) % top, axis=1)


def load_shares(amount, total, limit, skew, full):
    loads = [(1 << 20) // math.isqrt(standing ** skew) + 1 for standing in range(1, amount + 1)]
    largest = limit if full else min(limit, max(-(-total // amount), total * loads[0] // sum(loads)))
    least = 1 if total - largest >= amount - 1 else 0
    holding, spare = [largest] + [least] * (amount - 1), total - largest - least * (amount - 1)
    while spare > 0:
        candidates = [i for i in range(1, amount) if holding[i] < largest] or [i for i in range(1, amount) if holding[i] < limit]
        whole, left = sum([loads[i] for i in candidates]), spare
        for i in candidates:
            extra = min(limit - holding[i], max(1, left * loads[i] // whole), spare)
            holding[i] = holding[i] + extra
            spare = spare - extra
    return np.array(holding)


def centred(stream_key, shape, width, bound, cuts=(), kind=jnp.bfloat16):
    result = jax.random.normal(stream_key, shape, jnp.float32) * width
    if len(cuts) > 0:
        result = steps_of(stream_key, shape, cuts, -0.22, 0.18) * result
    return jnp.clip(result, min=-bound, max=bound).astype(kind)


def setup_inputs(seed: int = 0) -> dict:
    key_of = jax.random.split(jax.random.key(seed), 16)
    residual = centred(key_of[0], (TOKENS, D), 1.0, 6.0, ((0, 256),))
    queries = centred(key_of[1], (TOKENS, MIXER), 1.0, 6.0, ((0, 16), (1, 16)))
    keys = centred(key_of[2], (TOKENS, MIXER), 1.0, 6.0, ((0, 16), (1, 16)))
    values = centred(key_of[3], (TOKENS, MIXER), 1.0, 6.0, ((0, 16), (1, 16)))
    in_gate = draw_in_gate(jax.random.fold_in(key_of[15], 71), 0)
    forget_gate = draw_forget_gate(jax.random.fold_in(key_of[15], 71), 0)
    doc_ids = jnp.searchsorted(jnp.cumsum(uneven_parts(key_of[6], DOCS, TOKENS, TOKENS // 2, 2)), jnp.arange(TOKENS), side="right").astype(jnp.int32)
    head_gain = jnp.clip(1.0 + 0.18 * jax.random.normal(key_of[7], (MIXER,), jnp.float32), 0.1, 1.9)
    out_weight = centred(key_of[8], (MIXER, D), MIXER ** -0.5, 0.09375, ((0, 16),))
    norm_gain = jnp.clip(1.0 + 0.18 * jax.random.normal(key_of[9], (D,), jnp.float32), 0.1, 1.9)
    route_ids_keys = jax.random.split(jax.random.fold_in(key_of[10], 1), TOKENS // ROWS_DEV)
    route_ids_turns = jax.random.permutation(jax.random.fold_in(key_of[10], 3), TOKENS // ROWS_DEV)
    route_ids = jax.vmap(lambda own, number: shared_out(jax.random.fold_in(key_of[10], 2), own, number, ROWS_DEV, EXPERTS, TOPK, CAP, 2))(route_ids_keys, route_ids_turns).reshape((TOKENS, TOPK))
    route_weights = jnp.clip(0.2 + 0.8 * jax.random.uniform(key_of[11], (TOKENS, TOPK), jnp.float32) ** steps_of(key_of[11], (TOKENS, TOPK), ((0, 256),), -0.2, 0.2), 0.2, 1.0)
    gate_proj = centred(key_of[12], (EXPERTS, D, EXP_FF), D ** -0.5, 0.125, ((0, 16), (2, 16)))
    up_proj = centred(key_of[13], (EXPERTS, D, EXP_FF), D ** -0.5, 0.125, ((0, 16), (2, 16)))
    down_proj = centred(key_of[14], (EXPERTS, EXP_FF, D), EXP_FF ** -0.5, 0.09375, ((0, 16), (1, 16)))
    return dict(residual=residual, queries=queries, keys=keys, values=values, in_gate=in_gate, forget_gate=forget_gate, doc_ids=doc_ids, head_gain=head_gain, out_weight=out_weight, norm_gain=norm_gain, route_ids=route_ids, route_weights=route_weights, gate_proj=gate_proj, up_proj=up_proj, down_proj=down_proj)


MASKED = -1e+30
EPSILON = 1e-06

def block_step(state, pieces):
    memory, normalizer, max_level, carry_doc = state
    q_block, k_block, v_block, in_block, forget_block, doc_block = pieces
    scaling = q_block.shape[1] ** (-0.5)
    cum_forget = jnp.cumsum(forget_block)
    positions = jnp.arange(q_block.shape[0])
    permitted_mask = (positions[:, None] >= positions[None, :]) & (doc_block[:, None] == doc_block[None, :])
    log_weights = jnp.where(permitted_mask, cum_forget[:, None] - cum_forget[None, :] + in_block[None, :], MASKED)
    carried = jnp.where(doc_block == carry_doc, cum_forget + max_level, MASKED)
    row_max = jnp.maximum(carried, lax.optimization_barrier(jnp.max(log_weights, axis=1)))
    scores = jnp.dot(q_block, k_block.T, preferred_element_type=jnp.float32) * scaling
    weighted = scores * jnp.exp(log_weights - row_max[:, None])
    carry_weight = jnp.exp(carried - row_max)
    query_scaled = q_block.astype(jnp.float32) * scaling
    key_full = k_block.astype(jnp.float32)
    value_full = v_block.astype(jnp.float32)
    readout_numerator = jnp.dot(weighted, value_full, precision=lax.Precision.HIGHEST)
    readout_numerator = readout_numerator + carry_weight[:, None] * jnp.dot(query_scaled, memory.T, precision=lax.Precision.HIGHEST)
    denominator = lax.optimization_barrier(jnp.sum(weighted, axis=1)) + carry_weight * jnp.dot(query_scaled, normalizer, precision=lax.Precision.HIGHEST)
    last_doc = doc_block[-1]
    forget_total = cum_forget[-1]
    log_end = jnp.where(doc_block == last_doc, forget_total - cum_forget + in_block, MASKED)
    carry_log = jnp.where(carry_doc == last_doc, forget_total + max_level, MASKED)
    new_max = jnp.maximum(carry_log, jnp.max(log_end))
    end_weight = jnp.exp(log_end - new_max)
    kept_share = jnp.exp(carry_log - new_max)
    new_memory = kept_share * memory + jnp.dot((value_full * end_weight[:, None]).T, key_full, precision=lax.Precision.HIGHEST)
    new_normalizer = kept_share * normalizer + jnp.dot(end_weight, key_full, precision=lax.Precision.HIGHEST)
    return ((new_memory, new_normalizer, new_max, last_doc), (readout_numerator, denominator, row_max))

def run_blocks(queries_in, keys_in, incoming_vectors, in_gates, log_forget, doc_row, memory, normalizer, max_level, carry_doc):
    extent = queries_in.shape[0]
    block_size = math.gcd(extent, 256)
    blocks = extent // block_size

    def to_blocks(tensor):
        return tensor.reshape((blocks, block_size) + tensor.shape[1:])
    pieces = tuple((to_blocks(tensor) for tensor in (queries_in, keys_in, incoming_vectors, in_gates, log_forget, doc_row)))
    final_state, outputs = lax.scan(block_step, (memory, normalizer, max_level, carry_doc), pieces)
    readout_numerator, denominator, row_max = outputs
    return (readout_numerator.reshape(extent, -1), denominator.reshape(extent), row_max.reshape(extent), final_state)

def reference(residual, queries, keys, values, in_gate, forget_gate, doc_ids, head_gain, out_weight, norm_gain, route_ids, route_weights, gate_proj, up_proj, down_proj):

    def by_head(tensor):
        return tensor.reshape(TOKENS, STORE_ATTENDERS, HEAD).transpose(1, 0, 2)
    log_forget = jax.nn.log_sigmoid(forget_gate)
    run_heads = jax.vmap(run_blocks, in_axes=(0, 0, 0, 0, 0, None, 0, 0, 0, None))
    readout_numerator, denominator, row_max, unused = run_heads(by_head(queries), by_head(keys), by_head(values), in_gate, log_forget, doc_ids, jnp.zeros((STORE_ATTENDERS, HEAD, HEAD), jnp.float32), jnp.zeros((STORE_ATTENDERS, HEAD), jnp.float32), jnp.full((STORE_ATTENDERS,), MASKED, jnp.float32), doc_ids[0])
    mixed_heads = readout_numerator / jnp.maximum(jnp.abs(denominator), jnp.exp(-row_max))[..., None]
    normed_heads = mixed_heads * lax.rsqrt(lax.optimization_barrier(jnp.mean(mixed_heads * mixed_heads, axis=-1, keepdims=True)) + EPSILON)
    normed_heads = normed_heads * head_gain.reshape(STORE_ATTENDERS, 1, HEAD)
    head_rows = normed_heads.transpose(1, 0, 2).reshape(TOKENS, STORE_ATTENDERS * HEAD).astype(jnp.bfloat16)
    stream = residual.astype(jnp.float32) + jnp.dot(head_rows, out_weight, preferred_element_type=jnp.float32)
    normed = stream * lax.rsqrt(lax.optimization_barrier(jnp.mean(stream * stream, axis=-1, keepdims=True)) + EPSILON) * norm_gain
    normed = normed.astype(jnp.bfloat16)
    slice_width = EXP_FF // N_TP
    row_limit = N_SP * N_TP * CAP
    flat_ids = route_ids.reshape(-1)
    flat_weights = route_weights.reshape(-1)

    def per_expert(mix_total, pieces):
        gate_weight, up_weight, down_weight, expert = pieces
        chosen = flat_ids == expert
        slots_of = jnp.nonzero(chosen, size=row_limit, fill_value=0)[0].astype(jnp.int32)
        filled = jnp.arange(row_limit, dtype=jnp.int32) < jnp.sum(chosen.astype(jnp.int32))
        tokens_of = (slots_of // TOPK).astype(jnp.int32)
        weights_of = jnp.where(filled, flat_weights[slots_of], jnp.zeros((row_limit,), jnp.float32))
        rows_in = normed[tokens_of]
        gate_part = jnp.dot(rows_in, gate_weight, preferred_element_type=jnp.float32)
        up_part = jnp.dot(rows_in, up_weight, preferred_element_type=jnp.float32)
        hidden = (jax.nn.silu(gate_part) * up_part).astype(jnp.bfloat16)

        def added_portion(running, operands):
            hidden_slice, down_slice = operands
            partial_value = jnp.dot(hidden_slice, down_slice, preferred_element_type=jnp.float32).astype(jnp.bfloat16)
            partial_value = lax.optimization_barrier(partial_value)
            return (running + partial_value.astype(jnp.float32), None)
        summed, unused_out = lax.scan(added_portion, jnp.zeros((row_limit, D), jnp.float32), (hidden.reshape(row_limit, N_TP, slice_width).transpose(1, 0, 2), down_weight.reshape(N_TP, slice_width, D)))
        expert_out = summed.astype(jnp.bfloat16)
        return (mix_total.at[tokens_of].add(weights_of[:, None] * expert_out.astype(jnp.float32)), None)
    expert_mix, unused_all = lax.scan(per_expert, jnp.zeros((TOKENS, D), jnp.float32), (gate_proj, up_proj, down_proj, jnp.arange(EXPERTS, dtype=jnp.int32)))
    return (stream + expert_mix).astype(jnp.bfloat16)
```

```python
import jax
import jax.numpy as jnp
from jax import lax
from jax.experimental import pallas as pl
from jax.experimental.pallas import tpu as pltpu
from jax.sharding import PartitionSpec as P

MESH = pl.DeviceIdType.MESH
BF16 = jnp.bfloat16
F32 = jnp.float32
MASKED = -1e30
EPSILON = 1e-06
LANES = 128
CAP = 5
SLOTS = 8


def dot(a, b, contract=((1,), (0,))):
    return lax.dot_general(a, b, (contract, ((), ())), preferred_element_type=F32)


def halves_of(x):
    high = x.astype(BF16)
    return high, (x - high.astype(F32)).astype(BF16)


def column(row, extent):
    return jnp.transpose(jnp.broadcast_to(row, (LANES, extent)))


def wide(x, width):
    return jnp.concatenate([x] * (width // LANES), axis=1)


def barrier_with(peers):
    barrier = pltpu.get_barrier_semaphore()
    for peer in peers:
        pl.semaphore_signal(barrier, inc=1, device_id=peer, device_id_type=MESH)
    pl.semaphore_wait(barrier, len(peers))


def exchange_start(n, me, source, target, send_sem, recv_sem):
    copies = []
    for o in range(1, n):
        peer = lax.rem(me + o, n)
        copy = pltpu.make_async_remote_copy(
            src_ref=source.at[peer],
            dst_ref=target.at[me],
            send_sem=send_sem.at[o],
            recv_sem=recv_sem.at[o],
            device_id={"sp": peer},
            device_id_type=MESH,
        )
        copy.start()
        copies.append(copy)
    return copies


def mixer_kernel(
    n_sp,
    q_ref,
    k_ref,
    v_ref,
    in_ref,
    forget_ref,
    doc_ref,
    gain_ref,
    out_ref,
    own_state,
    all_states,
    prefixes,
    arrived,
    num_ref,
    den_ref,
    max_ref,
    send1,
    recv1,
    send2,
    recv2,
):
    me = lax.axis_index("sp")
    extent, head = q_ref.shape
    rows = head // n_sp
    scaling = head ** (-0.5)
    barrier_with([{"sp": lax.rem(me + o, n_sp)} for o in range(1, n_sp)])

    forget = forget_ref[...]
    small = jnp.exp(-jnp.abs(forget))
    above = 1.0 + small
    exact = above - 1.0
    log1p = jnp.where(exact == 0.0, small, jnp.log(above) * (small / jnp.where(exact == 0.0, 1.0, exact)))
    log_forget = jnp.minimum(forget, 0.0) - log1p
    cum = jnp.broadcast_to(log_forget, (8, extent))
    lane = lax.broadcasted_iota(jnp.int32, (8, extent), 1)
    shift = 1
    while shift < extent:
        cum = cum + jnp.where(lane >= shift, pltpu.roll(cum, shift, 1), 0.0)
        shift *= 2
    cum = cum[0:1]
    docs = doc_ref[...].astype(F32)
    base = in_ref[...] - cum
    total = cum[:, extent - 1 : extent]
    first_doc = docs[:, 0:1]
    last_doc = docs[:, extent - 1 : extent]
    log_end = jnp.where(docs == last_doc, total + base, MASKED)
    level = jnp.max(log_end, axis=1, keepdims=True)
    end_weight = column(jnp.exp(log_end - level), extent)
    forget_total = jnp.where(first_doc == last_doc, total, MASKED)

    keys = k_ref[...]
    weighted_values = jnp.concatenate(
        [v_ref[...].astype(F32) * wide(end_weight, head), end_weight], axis=1
    )
    high, low = halves_of(weighted_values)
    state = dot(keys, high, ((0,), (0,))) + dot(keys, low, ((0,), (0,)))
    tail_lane = lax.broadcasted_iota(jnp.int32, (head, LANES), 1)
    tail = state[:, head:]
    for at, scalar in ((1, level), (2, forget_total), (3, first_doc), (4, last_doc)):
        tail = jnp.where(tail_lane == at, scalar, tail)
    own_state[:, :, :head] = state[:, :head].reshape(n_sp, rows, head)
    own_state[:, :, head:] = tail.reshape(n_sp, rows, LANES)
    sends = exchange_start(n_sp, me, own_state, all_states, send1, recv1)
    all_states[me] = own_state[me]

    cum_col = column(cum, extent)
    doc_col = column(docs, extent)
    block = LANES
    for i in range(extent // block):
        here = slice(i * block, (i + 1) * block)
        width = (i + 1) * block
        scores = dot(q_ref[here, :], k_ref[:width, :], ((1,), (1,))) * scaling
        permitted = wide(doc_col[here], width) == docs[:, :width]
        row_at = lax.broadcasted_iota(jnp.int32, (block, width), 0) + i * block
        col_at = lax.broadcasted_iota(jnp.int32, (block, width), 1)
        permitted = permitted & (row_at >= col_at)
        logs = jnp.where(permitted, wide(cum_col[here], width) + base[:, :width], MASKED)
        row_max = jnp.max(logs, axis=1, keepdims=True)
        weighted = scores * jnp.exp(logs - row_max)
        num_ref[here, :] = dot(weighted.astype(BF16), v_ref[:width, :])
        den_ref[here, :] = jnp.broadcast_to(jnp.sum(weighted, axis=1, keepdims=True), (block, LANES))
        max_ref[here, :] = jnp.broadcast_to(row_max, (block, LANES))

    for copy in sends:
        copy.wait()
    running = jnp.zeros((rows, head + LANES), F32)
    running_level = jnp.full((rows, 1), MASKED, F32)
    running_doc = jnp.full((rows, 1), -1.0, F32)
    slice_lane = lax.broadcasted_iota(jnp.int32, (rows, LANES), 1)
    for j in range(n_sp):
        piece = all_states[j]
        piece_level = piece[:, head + 1 : head + 2]
        piece_forget = piece[:, head + 2 : head + 3]
        piece_first = piece[:, head + 3 : head + 4]
        in_level = jnp.where(running_doc == piece_first, running_level, MASKED)
        prefixes[j, :, :head] = running[:, :head]
        prefixes[j, :, head:] = jnp.where(slice_lane == 1, in_level, running[:, head:])
        passed = in_level + piece_forget
        running_level = jnp.maximum(passed, piece_level)
        running = jnp.exp(passed - running_level) * running + jnp.exp(piece_level - running_level) * jnp.concatenate(
            [piece[:, :head], jnp.where(slice_lane == 0, piece[:, head:], 0.0)], axis=1
        )
        running_doc = piece[:, head + 4 : head + 5]
    sends = exchange_start(n_sp, me, prefixes, arrived, send2, recv2)
    arrived[me] = prefixes[me]
    for copy in sends:
        copy.wait()

    in_level = arrived[0][0:1, head + 1 : head + 2]
    high, low = halves_of(arrived[...].reshape(head, head + LANES))
    gain = gain_ref[...]
    for i in range(extent // block):
        here = slice(i * block, (i + 1) * block)
        far = (dot(q_ref[here, :], high) + dot(q_ref[here, :], low)) * scaling
        carried = jnp.where(doc_col[here] == first_doc, cum_col[here] + in_level, MASKED)
        row_max = max_ref[here, :]
        new_max = jnp.maximum(row_max, carried)
        own_share = jnp.exp(row_max - new_max)
        far_share = jnp.exp(carried - new_max)
        numerator = wide(own_share, head) * num_ref[here, :] + wide(far_share, head) * far[:, :head]
        denominator = own_share * den_ref[here, :] + far_share * far[:, head : head + 1]
        bound = jnp.maximum(jnp.abs(denominator), jnp.exp(-new_max))
        mixed = numerator / wide(bound, head)
        scale = lax.rsqrt(jnp.mean(mixed * mixed, axis=1, keepdims=True) + EPSILON)
        out_ref[here, :] = (mixed * scale * gain).astype(BF16)


def ring_chains(n_z):
    far, near = n_z // 2, n_z // 2 - 1
    return ((1, 0, far), (1, 1, near), (-1, 0, near), (-1, 1, far))


def reduce_ring(n_z, z, core, part, half, out, inc, send_sem, recv_sem):
    chains = ring_chains(n_z)
    sent = {}
    for i in range(1, n_z // 2 + 1):
        for c, (way, h, steps) in enumerate(chains):
            if i > steps:
                continue
            cols = slice(h * half, (h + 1) * half)
            dest = lax.rem(z + way * (steps - i + 1) + n_z, n_z)
            value = part[dest, :, cols]
            if i > 1:
                sent[c, i - 1].wait_recv()
                value = value + inc[c, i - 2].astype(F32)
            out[c, i - 1] = value.astype(BF16)
            copy = pltpu.make_async_remote_copy(
                src_ref=out.at[c, i - 1],
                dst_ref=inc.at[c, i - 1],
                send_sem=send_sem.at[c, i - 1],
                recv_sem=recv_sem.at[c, i - 1],
                device_id={"tp": 2 * lax.rem(z + way + n_z, n_z) + core},
                device_id_type=MESH,
            )
            copy.start()
            sent[c, i] = copy
    sums = []
    for h in range(2):
        value = part[z, :, h * half : (h + 1) * half]
        for c, (way, chain_half, steps) in enumerate(chains):
            if chain_half == h:
                sent[c, steps].wait_recv()
                value = value + inc[c, steps - 1].astype(F32)
        sums.append(value)
    for copy in sent.values():
        copy.wait_send()
    return jnp.concatenate(sums, axis=1)


def expert_kernel(
    n_sp,
    n_z,
    heads_ref,
    residual_ref,
    norm_gain_ref,
    ids_ref,
    weights_ref,
    out_weight_ref,
    gate_ref,
    up_ref,
    down_ref,
    result_ref,
    w_out,
    w_gate,
    w_up,
    w_down,
    heads_in,
    part1,
    rs1_out,
    rs1_in,
    outgoing,
    incoming,
    gathered,
    part2,
    rs2_out,
    rs2_in,
    leaving,
    returned,
    local_sem,
    pair_send,
    pair_recv,
    rs1_send,
    rs1_recv,
    a2a_send,
    a2a_recv,
    ag_send,
    ag_recv,
    rs2_send,
    rs2_recv,
    back_send,
    back_recv,
):
    sp = lax.axis_index("sp")
    tp = lax.axis_index("tp")
    z = tp // 2
    core = tp - 2 * z
    sibling = {"tp": 2 * z + 1 - core}
    width = residual_ref.shape[1]
    half = width // 2
    tokens = residual_ref.shape[0]
    peers = [{"sp": lax.rem(sp + o, n_sp)} for o in range(1, n_sp)]
    peers += [sibling]
    peers += [{"tp": 2 * lax.rem(z + way + n_z, n_z) + core} for way in (1, -1)]
    barrier_with(peers)

    pair = []
    own = []
    moved = (
        (heads_ref.at[:, 1 - core], heads_in),
        (out_weight_ref, w_out.at[1]),
        (gate_ref, w_gate.at[1]),
        (up_ref, w_up.at[1]),
        (down_ref, w_down.at[1]),
    )
    for at, (source, target) in enumerate(moved):
        copy = pltpu.make_async_remote_copy(
            src_ref=source,
            dst_ref=target,
            send_sem=pair_send.at[at],
            recv_sem=pair_recv.at[at],
            device_id=sibling,
            device_id_type=MESH,
        )
        copy.start()
        pair.append(copy)
    for at, (source, target) in enumerate(
        (
            (out_weight_ref, w_out.at[0]),
            (gate_ref, w_gate.at[0]),
            (up_ref, w_up.at[0]),
            (down_ref, w_down.at[0]),
        )
    ):
        copy = pltpu.make_async_copy(source, target, local_sem.at[at])
        copy.start()
        own.append(copy)

    lane = lax.broadcasted_iota(jnp.int32, (tokens, LANES), 1)
    chosen = [ids_ref[:, k : k + 1] == lane for k in range(2)]
    either = jnp.where(chosen[0] | chosen[1], 1.0, 0.0)
    before = jnp.where(
        lax.broadcasted_iota(jnp.int32, (tokens, tokens), 0)
        > lax.broadcasted_iota(jnp.int32, (tokens, tokens), 1),
        1.0,
        0.0,
    )
    earlier = dot(before.astype(BF16), either.astype(BF16))
    select = []
    for k in range(2):
        rank = jnp.sum(jnp.where(chosen[k], earlier, 0.0), axis=1, keepdims=True)
        slot = ids_ref[:, k : k + 1].astype(F32) * SLOTS + rank
        select.append(jnp.where(slot == lane.astype(F32), 1.0, 0.0))

    own[0].wait()
    pair[0].wait()
    pair[1].wait()
    mine = heads_ref[:, core].reshape(n_z * tokens, -1)
    theirs = heads_in[...].reshape(n_z * tokens, -1)
    chunk = 512
    for at in range(0, width, chunk):
        cols = slice(at, at + chunk)
        part1[:, :, cols] = (dot(mine, w_out[0, :, cols]) + dot(theirs, w_out[1, :, cols])).reshape(
            n_z, tokens, chunk
        )
    update = reduce_ring(n_z, z, core, part1, half, rs1_out, rs1_in, rs1_send, rs1_recv)
    stream = residual_ref[...].astype(F32) + update
    normed = stream * lax.rsqrt(jnp.mean(stream * stream, axis=1, keepdims=True) + EPSILON)
    normed = (normed * norm_gain_ref[...]).astype(BF16)

    placed = dot((select[0] + select[1]).astype(BF16), normed, ((0,), (0,)))
    outgoing[...] = placed.reshape(n_sp, SLOTS, width).astype(BF16)
    sends = exchange_start(n_sp, sp, outgoing, incoming, a2a_send, a2a_recv)
    incoming[sp] = outgoing[sp]
    for copy in own[1:] + pair[2:]:
        copy.wait()
    for copy in sends:
        copy.wait()

    packed = n_sp * CAP
    padded = n_sp * SLOTS
    row = lax.broadcasted_iota(jnp.int32, (packed, padded), 0)
    col = lax.broadcasted_iota(jnp.int32, (packed, padded), 1)
    inside = jnp.bitwise_and(col, SLOTS - 1)
    source_row = jnp.right_shift(col, 3) * CAP + inside
    pack = jnp.where((source_row == row) & (inside < CAP), 1.0, 0.0).astype(BF16)
    padded_rows = incoming[...].astype(F32).reshape(padded, width).astype(BF16)
    packed_rows = dot(pack, padded_rows).astype(BF16)
    gathered[z, 0] = packed_rows[:, :half]
    gathered[z, 1] = packed_rows[:, half:]

    chains = ring_chains(n_z)
    gathers = {}

    def forward(c, i):
        way, h, steps = chains[c]
        if i > steps:
            return
        origin = lax.rem(z - way * (i - 1) + n_z, n_z)
        copy = pltpu.make_async_remote_copy(
            src_ref=gathered.at[origin, h],
            dst_ref=gathered.at[origin, h],
            send_sem=ag_send.at[c, i - 1],
            recv_sem=ag_recv.at[c, i - 1],
            device_id={"tp": 2 * lax.rem(z + way + n_z, n_z) + core},
            device_id_type=MESH,
        )
        copy.start()
        gathers[c, i] = copy

    def experts(origin):
        left = gathered[origin, 0]
        right = gathered[origin, 1]
        total = None
        for s in range(2):
            gate = dot(left, w_gate[s, :half, :]) + dot(right, w_gate[s, half:, :])
            up = dot(left, w_up[s, :half, :]) + dot(right, w_up[s, half:, :])
            hidden = (gate / (1.0 + jnp.exp(-gate)) * up).astype(BF16)
            down = dot(hidden, w_down[s])
            total = down if total is None else total + down
        part2[origin] = total

    for c in range(4):
        forward(c, 1)
    experts(z)
    for i in range(1, n_z // 2 + 1):
        for c, (way, h, steps) in enumerate(chains):
            if i <= steps:
                gathers[c, i].wait_recv()
                forward(c, i + 1)
        experts(lax.rem(z - i + n_z, n_z))
        if i < n_z // 2:
            experts(lax.rem(z + i, n_z))
    summed = reduce_ring(n_z, z, core, part2, half, rs2_out, rs2_in, rs2_send, rs2_recv)
    for copy in gathers.values():
        copy.wait_send()

    row = lax.broadcasted_iota(jnp.int32, (padded, packed), 0)
    col = lax.broadcasted_iota(jnp.int32, (padded, packed), 1)
    inside = jnp.bitwise_and(row, SLOTS - 1)
    source_row = jnp.right_shift(row, 3) * CAP + inside
    unpack = jnp.where((source_row == col) & (inside < CAP), 1.0, 0.0).astype(BF16)
    spread = dot(unpack, summed.astype(BF16))
    leaving[...] = spread.reshape(n_sp, SLOTS, width).astype(BF16)
    sends = exchange_start(n_sp, sp, leaving, returned, back_send, back_recv)
    returned[sp] = leaving[sp]
    for copy in sends:
        copy.wait()
    back = returned[...].astype(F32).reshape(padded, width).astype(BF16)
    total = stream
    for k in range(2):
        total = total + weights_ref[:, k : k + 1] * dot(select[k].astype(BF16), back)
    result_ref[...] = total.astype(BF16)


def on_device(
    n_sp,
    n_tp,
    residual,
    queries,
    keys,
    values,
    in_gate,
    forget_gate,
    doc_ids,
    head_gain,
    out_weight,
    norm_gain,
    route_ids,
    route_weights,
    gate_proj,
    up_proj,
    down_proj,
):
    extent, head = queries.shape
    rows = head // n_sp
    n_z = n_tp // 2
    tokens, width = residual.shape
    units = gate_proj.shape[2]
    vmem = pl.BlockSpec(memory_space=pltpu.VMEM)
    anywhere = pl.BlockSpec(memory_space=pl.ANY)
    dma = pltpu.SemaphoreType.DMA

    def body(*refs):
        mixer_kernel(n_sp, *refs)

    head_rows = pl.pallas_call(
        body,
        name="mixer",
        out_shape=jax.ShapeDtypeStruct((extent, head), BF16),
        in_specs=[vmem] * 7,
        out_specs=vmem,
        scratch_shapes=[pltpu.VMEM((n_sp, rows, head + LANES), F32)] * 4
        + [
            pltpu.VMEM((extent, head), F32),
            pltpu.VMEM((extent, LANES), F32),
            pltpu.VMEM((extent, LANES), F32),
        ]
        + [dma((n_sp,))] * 4,
        compiler_params=pltpu.CompilerParams(
            collective_id=0, has_side_effects=True, vmem_limit_bytes=48 << 20
        ),
    )(
        queries,
        keys,
        values,
        in_gate,
        forget_gate,
        doc_ids.reshape(1, extent),
        head_gain.reshape(1, head),
    )

    def body2(*refs):
        expert_kernel(n_sp, n_z, *refs)

    half = width // 2
    packed = n_sp * CAP
    steps = n_z // 2
    return pl.pallas_call(
        body2,
        name="experts",
        out_shape=jax.ShapeDtypeStruct((tokens, width), BF16),
        in_specs=[vmem] * 5 + [anywhere] * 4,
        out_specs=vmem,
        scratch_shapes=[
            pltpu.VMEM((2, head, width), BF16),
            pltpu.VMEM((2, width, units), BF16),
            pltpu.VMEM((2, width, units), BF16),
            pltpu.VMEM((2, units, width), BF16),
            pltpu.VMEM((n_z, tokens, head), BF16),
            pltpu.VMEM((n_z, tokens, width), F32),
            pltpu.VMEM((4, steps, tokens, half), BF16),
            pltpu.VMEM((4, steps, tokens, half), BF16),
            pltpu.VMEM((n_sp, SLOTS, width), BF16),
            pltpu.VMEM((n_sp, SLOTS, width), BF16),
            pltpu.VMEM((n_z, 2, packed, half), BF16),
            pltpu.VMEM((n_z, packed, width), F32),
            pltpu.VMEM((4, steps, packed, half), BF16),
            pltpu.VMEM((4, steps, packed, half), BF16),
            pltpu.VMEM((n_sp, SLOTS, width), BF16),
            pltpu.VMEM((n_sp, SLOTS, width), BF16),
            dma((4,)),
            dma((5,)),
            dma((5,)),
            dma((4, steps)),
            dma((4, steps)),
            dma((n_sp,)),
            dma((n_sp,)),
            dma((4, steps)),
            dma((4, steps)),
            dma((4, steps)),
            dma((4, steps)),
            dma((n_sp,)),
            dma((n_sp,)),
        ],
        compiler_params=pltpu.CompilerParams(
            collective_id=1, has_side_effects=True, vmem_limit_bytes=60 << 20
        ),
    )(
        head_rows.reshape(n_z, 2, tokens, head),
        residual,
        norm_gain.reshape(1, width),
        route_ids,
        route_weights,
        out_weight,
        gate_proj[0],
        up_proj[0],
        down_proj[0],
    )


def solution(mesh):
    n_sp, n_tp = mesh.shape["sp"], mesh.shape["tp"]
    both = ("sp", "tp")

    def step(*args):
        return on_device(n_sp, n_tp, *args)

    return jax.shard_map(
        step,
        mesh=mesh,
        in_specs=(
            P(both, None),
            P("sp", "tp"),
            P("sp", "tp"),
            P("sp", "tp"),
            P("tp", "sp"),
            P("tp", "sp"),
            P("sp"),
            P("tp"),
            P("tp", None),
            P(),
            P(both, None),
            P(both, None),
            P("sp", None, "tp"),
            P("sp", None, "tp"),
            P("sp", "tp", None),
        ),
        out_specs=P(both, None),
        check_vma=False,
    )
```
